512 devices in a mesh: fs: 16 (over z), rep: 4 (over y), tp: 8 (over x, core).
Axes of the slice: x: 4, y: 4, z: 16, core: 2. Of those that a mesh axis runs over, the one named last changes fastest.
Arguments:
- mixer_out: bfloat16 [65536, 1536], P(('fs', 'rep')), may hold values from -16 to 16
- out_grad: bfloat16 [65536, 4096], P(('fs', 'rep'), 'tp'), may hold values from -0.0234375 to 0.0234375
- factors: bfloat16 [1536, 256], P(('fs', 'rep')), may hold values from -0.15625 to 0.15625
- weight: float32 [1536, 4096], P(('fs', 'rep'), 'tp'), may hold values from -0.15625 to 0.15625
- first_moment: float32 [256, 4096], P(('fs', 'rep'), 'tp'), may hold values from -6 to 6
- second_moment: float32 [256, 4096], P(('fs', 'rep'), 'tp'), may hold values from 0.05 to 2
Outputs:
- new_weight: float32 [1536, 4096], P(('fs', 'rep'), 'tp')
- update: float32 [1536, 4096], P(('fs', 'rep'), 'tp')
- new_first: float32 [256, 4096], P(('fs', 'rep'), 'tp')
- new_second: float32 [256, 4096], P(('fs', 'rep'), 'tp')
- weight_copy: bfloat16 [1536, 4096], P(None, 'tp')
The draws below stay inside these ranges and needn't reach their ends.
All inputs are finite; a program needn't handle non-finite values.
Results may differ from the reference program's by a relative error of at most 0.0034.
Values may be sent and summed in bfloat16 or wider, within the bound.
A program may use at most 64 MiB of HBM per device.

```python
import math
import jax
import jax.numpy as jnp

D = 4096
DH = 1536
RANK = 256
TOK_DEV = 1024
TOKENS = 65536
N_FS = 16
N_REP = 4


def raised(result, rng, source, target, shards_of, factor):
    owner, partner = [(jnp.arange(result.shape[dim]) // (result.shape[dim] // shards_of)).reshape([-1 if axis == dim else 1 for axis in range(result.ndim)]) for dim in (source, target)]
    chosen = jax.random.permutation(rng, shards_of)[partner]
    strong = (owner == chosen) | (owner == (partner + shards_of // 2) % shards_of)
    return jnp.where(strong, factor * result, result)


def block_levels(own_key, dims, cuts, smallest, high):
    def one(axis_at, blocks):
        draws = jax.random.uniform(jax.random.fold_in(jax.random.fold_in(own_key, 6), axis_at), (blocks,), jnp.float32, smallest / len(cuts), high / len(cuts))
        return jnp.repeat(jnp.exp(draws), dims[axis_at] // blocks).reshape((-1,) + (1,) * (len(dims) - axis_at - 1))

    level = one(*cuts[0])
    for cut in cuts[1:]:
        level = level * one(*cut)
    return level


def noise(own_key, dims, scale, limit, pieces=(), dtype=jnp.bfloat16):
    drawn = jax.random.normal(own_key, dims, jnp.float32) * scale
    if len(pieces) > 0:
        drawn = block_levels(own_key, dims, pieces, -0.22, 0.18) * drawn
    return jnp.clip(drawn, min=-limit, max=limit).astype(dtype)


def bell_draw_with(stream_key, dims, spread, most, pieces, heavy, kind=jnp.bfloat16):
    entries = spread * jax.random.normal(stream_key, dims, jnp.float32)
    if pieces:
        entries = entries * block_levels(stream_key, dims, pieces, -0.22, 0.18)
    return jnp.clip(raised(entries, jax.random.fold_in(stream_key, 3), *heavy), -most, most).astype(kind)


def setup_inputs(seed: int = 0) -> dict:
    arg_keys = jax.random.split(jax.random.key(seed), 7)
    return {
        "mixer_out": bell_draw_with(arg_keys[0], (TOKENS, DH), 1.0, 16.0, ((0, 64),), (0, 1, 64, 4.0)),
        "out_grad": noise(arg_keys[1], (TOKENS, D), ((TOK_DEV * N_FS * N_REP) ** -0.5), 0.0234375, ((0, 64), (1, 8))),
        "factors": noise(arg_keys[2], (DH, RANK), DH ** -0.5, 0.15625, ((0, 64),)),
        "weight": noise(arg_keys[3], (DH, D), DH ** -0.5, 0.15625, ((0, 64), (1, 8)), jnp.float32),
        "first_moment": noise(arg_keys[4], (RANK, D), 1.0, 6.0, ((0, 64), (1, 8)), jnp.float32),
        "second_moment": jnp.clip(jnp.exp(math.log(2.0) - 3.6888794 * jax.random.uniform(arg_keys[5], (RANK, D), jnp.float32) ** block_levels(arg_keys[5], (RANK, D), ((0, 64), (1, 8)), -0.2, 0.2)), 0.05, 2.0),
    }


def reference(mixer_out, out_grad, factors, weight, first_moment, second_moment):
    gradient = jnp.dot(mixer_out.T, out_grad, preferred_element_type=jnp.float32)
    grad_low = gradient.astype(jnp.bfloat16)
    projected = jnp.dot(factors.T, grad_low, preferred_element_type=jnp.float32)
    new_first = 0.8 * first_moment + 0.2 * projected
    new_second = 0.9 * second_moment + 0.1 * projected * projected
    direction = new_first / (jnp.sqrt(new_second) + 1e-08)
    dir_low = direction.astype(jnp.bfloat16)
    proj_low = projected.astype(jnp.bfloat16)
    dir_wide = dir_low.astype(jnp.float32)
    proj_wide = proj_low.astype(jnp.float32)
    scale_ratio = jnp.sqrt(jnp.sum(dir_wide * dir_wide)) / jnp.sqrt(jnp.sum(proj_wide * proj_wide) + 1e-06)
    back_dir = jnp.dot(factors, dir_low, preferred_element_type=jnp.float32)
    back_proj = jnp.dot(factors, proj_low, preferred_element_type=jnp.float32)
    update = back_dir + scale_ratio * (gradient - back_proj)
    new_weight = weight - 0.01 * update
    weight_copy = new_weight.astype(jnp.bfloat16)
    return (new_weight, update, new_first, new_second, weight_copy)
```

```python
import jax
import jax.numpy as jnp
from jax import lax
from jax.experimental import pallas as pl
from jax.experimental.pallas import tpu as pltpu
from jax.sharding import PartitionSpec as P

MESH = pl.DeviceIdType.MESH
F32, BF16 = jnp.float32, jnp.bfloat16
WINDOW = ((1, 15, 2), (1, 15, 14))
YS = (1, 3, 2)
N_SEM = 160


def pack(v):
    low = jnp.concatenate([v[16:24, 0:128], v[16:24, 128:256]], axis=0)
    return jnp.concatenate([v[0:16], low], axis=1)


def unpack(v):
    low = jnp.concatenate([v[0:8, 256:384], v[8:16, 256:384]], axis=1)
    return jnp.concatenate([v[0:16, 0:256], low], axis=0)


def rows_dot(a, b):
    return lax.dot_general(a, b, (((0,), (0,)), ((), ())), preferred_element_type=F32)


def kernel(mixer, og, fac, w, m1, m2, nw_o, up_o, nf_o, ns_o, wc_o,
           gf, sy, ry, gy, sa, ra, ga, sb, rb, fall, f32s, pp, spy, rpy, spa, rpa, pb, m1a, m2a, dall, pick, mom, sums,
           wall, ssem, rsem):
    z, y, t = lax.axis_index("fs"), lax.axis_index("rep"), lax.axis_index("tp")
    q, r = z // 4, lax.rem(z, 4)

    def zd(d):
        return {"fs": lax.rem(z + d, 16)}

    def yd(d):
        return {"rep": lax.rem(y + d, 4)}

    def td(d):
        return {"tp": lax.rem(t + d, 8)}

    copies = []

    def send(src, dst, dev):
        i = len(copies)
        c = pltpu.make_async_remote_copy(src_ref=src, dst_ref=dst, send_sem=ssem.at[i], recv_sem=rsem.at[i],
                                         device_id=dev, device_id_type=MESH)
        c.start()
        copies.append(c)
        return c

    def rows(index, size):
        return pl.ds(pl.multiple_of(index * size, size), size)

    barrier = pltpu.get_barrier_semaphore()
    peers = [zd(d) for d in (1, 15, 2, 14, 4, 8, 12)] + [yd(d) for d in YS] + [td(d) for d in range(1, 8)]
    for dev in peers:
        pl.semaphore_signal(barrier, inc=1, device_id=dev, device_id_type=MESH)
    pl.semaphore_wait(barrier, len(peers))

    m1a[q] = m1[...]
    m2a[q] = m2[...]
    src = lax.broadcasted_iota(jnp.int32, (256, 256), 0)
    dst = lax.broadcasted_iota(jnp.int32, (256, 256), 1)
    ky = dst // 64
    rest = dst - ky * 64
    kr = rest // 16
    rest = rest - kr * 16
    kk = rest // 4
    order = kk * 64 + kr * 16 + ky * 4 + (rest - kk * 4)
    swap = jnp.where(src == order, 1.0, 0.0).astype(BF16)
    fac_p = jnp.dot(fac[...], swap, preferred_element_type=F32)
    fall[r, q] = pack(fac_p).astype(BF16)
    fb, mb = [], []
    for j in (1, 3, 2):
        fb.append(send(fall.at[r, q], fall.at[r, q], zd(4 * j)))
    for j in (1, 3, 2):
        mb.append(send(m1a.at[q], m1a.at[q], zd(4 * j)))
        mb.append(send(m2a.at[q], m2a.at[q], zd(4 * j)))

    for k in range(4):
        tile = rows_dot(mixer[:, 384 * k:384 * k + 384], og[...])
        for rr in range(4):
            for yy in range(4):
                at = 96 * rr + 24 * yy
                to = yy * 384 + rr * 96 + k * 24
                for c in range(2):
                    gf[c, to:to + 24, :] = tile[at:at + 24, 256 * c:256 * c + 256]
    gy_copies = []
    for c in range(2):
        sy[c] = gf[c].astype(BF16)
        gy_copies.append([send(sy.at[c, rows(lax.rem(y + d, 4), 384)], ry.at[c, j], yd(d)) for j, d in enumerate(YS)])

    for c in fb:
        c.wait_recv()
    fa = [send(fall.at[r], fall.at[r], zd(1)), send(fall.at[r], fall.at[r], zd(15)),
          send(fall.at[r, pl.ds(0, 2)], fall.at[r, pl.ds(0, 2)], zd(2)),
          send(fall.at[r, pl.ds(2, 2)], fall.at[r, pl.ds(2, 2)], zd(14))]
    for c in fa:
        c.wait_recv()
    for rr in range(4):
        for k in range(4):
            f32s[rr * 96 + k * 24:rr * 96 + k * 24 + 24, :] = unpack(fall[rr, k].astype(F32))
    fy = f32s[...].astype(BF16)

    ga_copies, py_copies = [], []
    for c in range(2):
        for x in gy_copies[c]:
            x.wait_recv()
        total = gf[c, rows(y, 384), :]
        for j in range(3):
            total = total + ry[c, j].astype(F32)
        gy[c] = total
        low = total.astype(BF16)
        sa[c] = low
        part = rows_dot(fy, low)
        pp[c] = part
        spy[c] = part.astype(BF16)
        py_copies.append([send(spy.at[c, rows(lax.rem(y + d, 4), 64)], rpy.at[c, j], yd(d)) for j, d in enumerate(YS)])
        ga_copies.append([send(sa.at[c, rows(lax.rem(z + d, 4), 96)], ra.at[c, j], zd(d))
                          for j, d in enumerate(WINDOW[c])])

    pa_copies, pb_copies, gb_copies = [], [], []
    for c in range(2):
        for x in py_copies[c]:
            x.wait_recv()
        total = pp[c, rows(y, 64), :]
        for j in range(3):
            total = total + rpy[c, j].astype(F32)
        spa[c] = total
        pa_copies.append([send(spa.at[c, rows(lax.rem(z + d, 4), 16)], rpa.at[c, j], zd(d))
                          for j, d in enumerate(WINDOW[c])])
    for c in range(2):
        for x in pa_copies[c]:
            x.wait_recv()
        total = spa[c, rows(r, 16), :]
        for j in range(3):
            total = total + rpa[c, j]
        pb[c, q] = total
        pb_copies.append([send(pb.at[c, q], pb.at[c, q], zd(4 * j)) for j in (1, 3, 2)])
        for x in ga_copies[c]:
            x.wait_recv()
        total = gy[c, rows(r, 96), :]
        for j in range(3):
            total = total + ra[c, j].astype(F32)
        ga[c] = total
        for k in range(4):
            sb[c, k] = pack(total[24 * k:24 * k + 24]).astype(BF16)
        gb_copies.append([send(sb.at[c, lax.rem(q + j, 4)], rb.at[c, j - 1], zd(4 * j)) for j in (1, 3, 2)])

    for x in mb:
        x.wait_recv()
    proj = []
    for c in range(2):
        for x in pb_copies[c]:
            x.wait_recv()
        proj.append(((pb[c, 0] + pb[c, 1]) + pb[c, 2]) + pb[c, 3])
    proj = jnp.concatenate(proj, axis=1)
    for k in range(4):
        pick[0, 4 * k:4 * k + 4, :] = m1a[k]
        pick[1, 4 * k:4 * k + 4, :] = m2a[k]
    first = 0.8 * pick[0] + 0.2 * proj
    second = 0.9 * pick[1] + 0.1 * proj * proj
    direction = first / (jnp.sqrt(second) + 1e-08)
    dall[0, y, r] = direction.astype(BF16)
    dall[1, y, r] = proj.astype(BF16)
    da = []
    for d in (1, 15):
        for p in range(2):
            da.append(send(dall.at[p, y, r], dall.at[p, y, r], zd(d)))
    for d, at in ((2, 0), (14, 256)):
        for p in range(2):
            here = dall.at[p, y, r, :, pl.ds(at, 256)]
            da.append(send(here, here, zd(d)))
    for k in range(4):
        mom[0, k] = first[4 * k:4 * k + 4]
        mom[1, k] = second[4 * k:4 * k + 4]
    nf_o[...] = mom[0, q]
    ns_o[...] = mom[1, q]
    for x in da:
        x.wait_recv()
    dy = [send(dall.at[p, y], dall.at[p, y], yd(d)) for d in YS for p in range(2)]

    grad = []
    for c in range(2):
        for x in gb_copies[c]:
            x.wait_recv()
        total = ga[c, rows(q, 24), :]
        for j in range(3):
            total = total + unpack(rb[c, j].astype(F32))
        grad.append(total)
    grad = jnp.concatenate(grad, axis=1)

    for x in dy:
        x.wait_recv()
    both = []
    for p in range(2):
        both.append(dall[p].reshape(256, 512))
        wide = both[p].astype(F32)
        sq = (wide * wide).reshape(32, 8, 512).sum(axis=0)
        sums[t, p] = sq[:, 0:128] + sq[:, 128:256] + sq[:, 256:384] + sq[:, 384:512]
    st = [send(sums.at[t], sums.at[t], td(d)) for d in range(1, 8)]
    mine = fac_p.astype(BF16)
    back_dir = jnp.dot(mine, both[0], preferred_element_type=F32)
    back_proj = jnp.dot(mine, both[1], preferred_element_type=F32)
    for x in st:
        x.wait_recv()
    totals = []
    for p in range(2):
        s = sums[0, p]
        for i in range(1, 8):
            s = s + sums[i, p]
        totals.append(jnp.sum(jnp.sum(s, axis=1, keepdims=True), axis=0, keepdims=True))
    scale = jnp.sqrt(totals[0]) / jnp.sqrt(totals[1] + 1e-06)
    update = back_dir + scale * (grad - back_proj)
    up_o[...] = update
    new_w = w[...] - 0.01 * update
    nw_o[...] = new_w
    wall[y, r, q] = jnp.concatenate([pack(new_w[:, 0:256]), pack(new_w[:, 256:512])], axis=1).astype(BF16)

    def block(dz, j):
        zz = lax.rem(z + 16 - dz, 16)
        return lax.rem(zz, 4), lax.rem(zz // 4 + 4 - j, 4)

    last = []

    def spread(rr, kk):
        for d in YS:
            last.append(send(wall.at[y, rr, kk], wall.at[y, rr, kk], yd(d)))

    first_b = {j: send(wall.at[y, r, q], wall.at[y, r, q], zd(4 * j)) for j in (2, 1, 3)}
    second_a = {}

    def around(j):
        rr, kk = block(0, j)
        to = {0: (1, 15, 2, 14), 1: (1, 15, 2), 3: (1, 15, 14), 2: (1, 15)}[j]
        for d in to:
            second_a[j, d] = send(wall.at[y, rr, kk], wall.at[y, rr, kk], zd(d))
        return to

    def landed(j, to):
        for d in to:
            second_a[j, d].wait_recv()
            spread(*block(d, j))

    to = around(0)
    spread(r, q)
    landed(0, to)
    for j in (1, 3):
        first_b[j].wait_recv()
        to = around(j)
        spread(*block(0, j))
        landed(j, to)
    first_b[2].wait_recv()
    to = around(2)
    spread(*block(0, 2))
    landed(2, to)
    for x in last:
        x.wait_recv()
    for k in range(4):
        for rr in range(4):
            at = 96 * (4 * k + rr)
            out = []
            for yy in range(4):
                v = wall[yy, rr, k].astype(F32)
                out.append(jnp.concatenate([unpack(v[:, 0:384]), unpack(v[:, 384:768])], axis=1))
            wc_o[at:at + 96, :] = jnp.concatenate(out, axis=0).astype(BF16)
    for x in copies:
        x.wait_send()


def per_device(*args):
    v = pl.BlockSpec(memory_space=pltpu.VMEM)
    shape = jax.ShapeDtypeStruct
    return pl.pallas_call(
        kernel,
        name="step",
        out_shape=(shape((24, 512), F32), shape((24, 512), F32), shape((4, 512), F32), shape((4, 512), F32),
                   shape((1536, 512), BF16)),
        in_specs=[v] * 6,
        out_specs=[v] * 5,
        scratch_shapes=[
            pltpu.VMEM((2, 1536, 256), F32),
            pltpu.VMEM((2, 1536, 256), BF16),
            pltpu.VMEM((2, 3, 384, 256), BF16),
            pltpu.VMEM((2, 384, 256), F32),
            pltpu.VMEM((2, 384, 256), BF16),
            pltpu.VMEM((2, 3, 96, 256), BF16),
            pltpu.VMEM((2, 96, 256), F32),
            pltpu.VMEM((2, 4, 16, 384), BF16),
            pltpu.VMEM((2, 3, 16, 384), BF16),
            pltpu.VMEM((4, 4, 16, 384), BF16),
            pltpu.VMEM((384, 256), F32),
            pltpu.VMEM((2, 256, 256), F32),
            pltpu.VMEM((2, 256, 256), BF16),
            pltpu.VMEM((2, 3, 64, 256), BF16),
            pltpu.VMEM((2, 64, 256), F32),
            pltpu.VMEM((2, 3, 16, 256), F32),
            pltpu.VMEM((2, 4, 16, 256), F32),
            pltpu.VMEM((4, 4, 512), F32),
            pltpu.VMEM((4, 4, 512), F32),
            pltpu.VMEM((2, 4, 4, 16, 512), BF16),
            pltpu.VMEM((2, 16, 512), F32),
            pltpu.VMEM((2, 4, 4, 512), F32),
            pltpu.VMEM((8, 2, 8, 128), F32),
            pltpu.VMEM((4, 4, 4, 16, 768), BF16),
            pltpu.SemaphoreType.DMA((N_SEM,)),
            pltpu.SemaphoreType.DMA((N_SEM,)),
        ],
        compiler_params=pltpu.CompilerParams(collective_id=0, has_side_effects=True, vmem_limit_bytes=56 * 1024 * 1024),
    )(*args)


def solution(mesh):
    both = ("fs", "rep")
    in_specs = (P(both, None), P(both, "tp"), P(both, None), P(both, "tp"), P(both, "tp"), P(both, "tp"))
    out_specs = (P(both, "tp"), P(both, "tp"), P(both, "tp"), P(both, "tp"), P(None, "tp"))
    return jax.shard_map(per_device, mesh=mesh, in_specs=in_specs, out_specs=out_specs, check_vma=False)
```

```python
import jax
import jax.numpy as jnp
from jax import lax
from jax.experimental import pallas as pl
from jax.experimental.pallas import tpu as pltpu
from jax.sharding import PartitionSpec as P

MESH = pl.DeviceIdType.MESH
F32, BF16 = jnp.float32, jnp.bfloat16
WINDOW = ((1, 15, 2), (1, 15, 14))
YS = (1, 3, 2)
N_SEM = 192


def pack(v):
    low = jnp.concatenate([v[16:24, 0:128], v[16:24, 128:256]], axis=0)
    return jnp.concatenate([v[0:16], low], axis=1)


def unpack(v):
    low = jnp.concatenate([v[0:8, 256:384], v[8:16, 256:384]], axis=1)
    return jnp.concatenate([v[0:16, 0:256], low], axis=0)


def rows_dot(a, b):
    return lax.dot_general(a, b, (((0,), (0,)), ((), ())), preferred_element_type=F32)


def kernel(mixer_h, og_h, fac_h, w_h, m1_h, m2_h, out_o, wc_o,
           mixer, og, fac, w, mom, turned, gf, sy, relay, direct, joined, landed_j, gy, sa, ra, ga, sb, rb, fall, f32s,
           pp, spy, rpy, spa, rpa, pb, m1a, m2a, dall, pick, sums, klass, ysum, wall, isem, ssem, rsem):
    z, y, t = lax.axis_index("fs"), lax.axis_index("rep"), lax.axis_index("tp")
    q, r = z // 4, lax.rem(z, 4)

    def zd(d):
        return {"fs": lax.rem(z + d, 16)}

    def yd(d):
        return {"rep": lax.rem(y + d, 4)}

    def td(d):
        return {"tp": lax.rem(t + d, 8)}

    copies = []

    def send(src, dst, dev):
        i = len(copies)
        c = pltpu.make_async_remote_copy(src_ref=src, dst_ref=dst, send_sem=ssem.at[i], recv_sem=rsem.at[i],
                                         device_id=dev, device_id_type=MESH)
        c.start()
        copies.append(c)
        return c

    def rows(index, size):
        return pl.ds(pl.multiple_of(index * size, size), size)

    barrier = pltpu.get_barrier_semaphore()
    peers = [zd(d) for d in (1, 15, 2, 14, 4, 8, 12)] + [yd(d) for d in YS] + [td(d) for d in range(1, 8)]
    for dev in peers:
        pl.semaphore_signal(barrier, inc=1, device_id=dev, device_id_type=MESH)

    def load(i, src, dst):
        c = pltpu.make_async_copy(src, dst, isem.at[i])
        c.start()
        return c

    tiles = [pl.ds(384 * k, 384) for k in range(4)]
    in_og = load(0, og_h, og)
    in_mixer = [load(1 + k, mixer_h.at[:, tiles[k]], mixer.at[:, tiles[k]]) for k in range(4)]
    in_fac = load(5, fac_h, fac)
    in_m1 = load(6, m1_h, m1a.at[q])
    in_m2 = load(7, m2_h, m2a.at[q])
    in_w = load(8, w_h, w)

    def partial(c):
        cols = pl.ds(256 * c, 256)
        for k in range(4):
            if c == 0:
                in_mixer[k].wait()
                turned[k] = mixer[:, tiles[k]].T
            tile = jnp.dot(turned[k], og[:, cols], preferred_element_type=F32)
            for rr in range(4):
                for yy in range(4):
                    at = 96 * rr + 24 * yy
                    to = yy * 384 + rr * 96 + k * 24
                    gf[c, to:to + 24, :] = tile[at:at + 24]
        sy[c] = gf[c].astype(BF16)

    in_og.wait()
    partial(0)
    in_fac.wait()

    src = lax.broadcasted_iota(jnp.int32, (256, 256), 0)
    dst = lax.broadcasted_iota(jnp.int32, (256, 256), 1)
    ky = dst // 64
    rest = dst - ky * 64
    kr = rest // 16
    rest = rest - kr * 16
    kk = rest // 4
    order = kk * 64 + kr * 16 + ky * 4 + (rest - kk * 4)
    swap = jnp.where(src == order, 1.0, 0.0).astype(BF16)
    fac_p = jnp.dot(fac[...], swap, preferred_element_type=F32)
    fall[r, q] = pack(fac_p).astype(BF16)
    in_m1.wait()
    in_m2.wait()
    pl.semaphore_wait(barrier, len(peers))

    def piece(d, half):
        return pl.ds(pl.multiple_of(lax.rem(y + d, 4) * 384 + 192 * half, 192), 192)

    def step_one(c):
        up = [send(sy.at[c, piece(2, 0)], relay.at[c, 0], yd(1)), send(sy.at[c, piece(1, 1)], direct.at[c, 0], yd(1))]
        down = [send(sy.at[c, piece(2, 1)], relay.at[c, 1], yd(3)), send(sy.at[c, piece(3, 0)], direct.at[c, 1], yd(3))]
        return up[0], down[0], up[1], down[1]

    def step_two(c, first):
        out = []
        for i, d in ((0, 1), (1, 3)):
            first[i].wait_recv()
            joined[c, i] = (gf[c, piece(d, i), :] + relay[c, i].astype(F32)).astype(BF16)
            out.append(send(joined.at[c, i], landed_j.at[c, i], yd(d)))
        return list(first[2:]) + out

    ones, twos = [None, None], [None, None]
    ones[0] = step_one(0)
    fb, mb = [], []
    for j in (1, 3, 2):
        fb.append(send(fall.at[r, q], fall.at[r, q], zd(4 * j)))
    for j in (1, 3, 2):
        mb.append(send(m1a.at[q], m1a.at[q], zd(4 * j)))
        mb.append(send(m2a.at[q], m2a.at[q], zd(4 * j)))
    partial(1)
    twos[0] = step_two(0, ones[0])
    ones[1] = step_one(1)

    for c in fb:
        c.wait_recv()
    fa = [send(fall.at[r], fall.at[r], zd(1)), send(fall.at[r], fall.at[r], zd(15)),
          send(fall.at[r, pl.ds(0, 2)], fall.at[r, pl.ds(0, 2)], zd(2)),
          send(fall.at[r, pl.ds(2, 2)], fall.at[r, pl.ds(2, 2)], zd(14))]
    for c in fa:
        c.wait_recv()
    for rr in range(4):
        for k in range(4):
            f32s[rr * 96 + k * 24:rr * 96 + k * 24 + 24, :] = unpack(fall[rr, k].astype(F32))
    fy = f32s[...].astype(BF16)

    ga_copies, py_copies = [], []
    for c in range(2):
        if c == 1:
            twos[1] = step_two(1, ones[1])
        for x in twos[c]:
            x.wait_recv()
        total = jnp.concatenate(
            [gf[c, piece(0, 0), :] + landed_j[c, 0].astype(F32) + direct[c, 1].astype(F32),
             gf[c, piece(0, 1), :] + landed_j[c, 1].astype(F32) + direct[c, 0].astype(F32)], axis=0)
        gy[c] = total
        low = total.astype(BF16)
        sa[c] = low
        part = rows_dot(fy, low)
        pp[c] = part
        spy[c] = part.astype(BF16)
        py_copies.append([send(spy.at[c, rows(lax.rem(y + d, 4), 64)], rpy.at[c, j], yd(d)) for j, d in enumerate(YS)])
        ga_copies.append([send(sa.at[c, rows(lax.rem(z + d, 4), 96)], ra.at[c, j], zd(d))
                          for j, d in enumerate(WINDOW[c])])

    pa_copies, pb_copies, gb_copies = [], [], []
    for c in range(2):
        for x in py_copies[c]:
            x.wait_recv()
        total = pp[c, rows(y, 64), :]
        for j in range(3):
            total = total + rpy[c, j].astype(F32)
        spa[c] = total
        pa_copies.append([send(spa.at[c, rows(lax.rem(z + d, 4), 16)], rpa.at[c, j], zd(d))
                          for j, d in enumerate(WINDOW[c])])
    for c in range(2):
        for x in pa_copies[c]:
            x.wait_recv()
        total = spa[c, rows(r, 16), :]
        for j in range(3):
            total = total + rpa[c, j]
        pb[c, q] = total
        pb_copies.append([send(pb.at[c, q], pb.at[c, q], zd(4 * j)) for j in (1, 3, 2)])
        for x in ga_copies[c]:
            x.wait_recv()
        total = gy[c, rows(r, 96), :]
        for j in range(3):
            total = total + ra[c, j].astype(F32)
        ga[c] = total
        for k in range(4):
            sb[c, k] = pack(total[24 * k:24 * k + 24]).astype(BF16)
        gb_copies.append([send(sb.at[c, lax.rem(q + j, 4)], rb.at[c, j - 1], zd(4 * j)) for j in (1, 3, 2)])

    for x in mb:
        x.wait_recv()
    proj = []
    for c in range(2):
        for x in pb_copies[c]:
            x.wait_recv()
        proj.append(((pb[c, 0] + pb[c, 1]) + pb[c, 2]) + pb[c, 3])
    proj = jnp.concatenate(proj, axis=1)
    for k in range(4):
        pick[0, 4 * k:4 * k + 4, :] = m1a[k]
        pick[1, 4 * k:4 * k + 4, :] = m2a[k]
    first = 0.8 * pick[0] + 0.2 * proj
    second = 0.9 * pick[1] + 0.1 * proj * proj
    direction = first / (jnp.sqrt(second) + 1e-08)
    dall[0, y, r] = direction.astype(BF16)
    dall[1, y, r] = proj.astype(BF16)
    da = {}
    for d in (1, 15):
        da[d] = [send(dall.at[p, y, r], dall.at[p, y, r], zd(d)) for p in range(2)]
    for d, at in ((2, 0), (14, 256)):
        here = [dall.at[p, y, r, :, pl.ds(at, 256)] for p in range(2)]
        da[d] = [send(here[p], here[p], zd(d)) for p in range(2)]
    dy = []

    def on(rr):
        for d in YS:
            for p in range(2):
                dy.append(send(dall.at[p, y, rr], dall.at[p, y, rr], yd(d)))

    for p in range(2):
        wide = dall[p, y, r].astype(F32)
        sq = wide * wide
        sq = sq[0:8] + sq[8:16]
        sums[t, p] = sq[:, 0:128] + sq[:, 128:256] + sq[:, 256:384] + sq[:, 384:512]
    st = [send(sums.at[t], sums.at[t], td(d)) for d in range(1, 8)]
    on(r)
    for k in range(4):
        mom[0, k] = first[4 * k:4 * k + 4]
        mom[1, k] = second[4 * k:4 * k + 4]
    out_o[48:52, :] = mom[0, q]
    out_o[52:56, :] = mom[1, q]
    for x in st:
        x.wait_recv()
    s = sums[0]
    for i in range(1, 8):
        s = s + sums[i]
    klass[r] = s
    sa_copies = [send(klass.at[r], klass.at[r], zd(d)) for d in (1, 15, 2)]
    for d in (1, 15):
        for x in da[d]:
            x.wait_recv()
        on(lax.rem(z + 16 - d, 4))
    for d in (2, 14):
        for x in da[d]:
            x.wait_recv()
    on(lax.rem(z + 2, 4))
    for x in sa_copies:
        x.wait_recv()
    ysum[y] = ((klass[0] + klass[1]) + klass[2]) + klass[3]
    sy_copies = [send(ysum.at[y], ysum.at[y], yd(d)) for d in YS]

    grad = []
    for c in range(2):
        for x in gb_copies[c]:
            x.wait_recv()
        total = ga[c, rows(q, 24), :]
        for j in range(3):
            total = total + unpack(rb[c, j].astype(F32))
        grad.append(total)
    grad = jnp.concatenate(grad, axis=1)
    mine = fac_p.astype(BF16)
    in_w.wait()

    for x in dy:
        x.wait_recv()
    both = [dall[p].reshape(256, 512) for p in range(2)]
    back_dir = jnp.dot(mine, both[0], preferred_element_type=F32)
    back_proj = jnp.dot(mine, both[1], preferred_element_type=F32)
    for x in sy_copies:
        x.wait_recv()
    s = ((ysum[0] + ysum[1]) + ysum[2]) + ysum[3]
    totals = [jnp.sum(jnp.sum(s[p], axis=1, keepdims=True), axis=0, keepdims=True) for p in range(2)]
    scale = jnp.sqrt(totals[0]) / jnp.sqrt(totals[1] + 1e-06)
    update = back_dir + scale * (grad - back_proj)
    out_o[0:24, :] = update
    new_w = w[...] - 0.01 * update
    out_o[24:48, :] = new_w
    wall[y, r, q] = jnp.concatenate([pack(new_w[:, 0:256]), pack(new_w[:, 256:512])], axis=1).astype(BF16)

    def block(dz, j):
        zz = lax.rem(z + 16 - dz, 16)
        return lax.rem(zz, 4), lax.rem(zz // 4 + 4 - j, 4)

    spread, onward = [], []

    def to_y(rr, kk):
        here = wall.at[y, rr, kk]
        spread.append((send(here, here, yd(1)), send(here, here, yd(3)), rr, kk))

    def pass_on(n):
        for _ in range(n):
            i = len(onward)
            up, down, rr, kk = spread[i]
            for c in (up, down):
                c.wait_recv()
            here = wall.at[lax.rem(y + (1 if i % 2 else 3), 4), rr, kk]
            onward.append(send(here, here, yd(3 if i % 2 else 1)))

    first_b = {j: send(wall.at[y, r, q], wall.at[y, r, q], zd(4 * j)) for j in (2, 1, 3)}
    second_a = {}

    def around(j):
        rr, kk = block(0, j)
        to = {0: (1, 15, 2, 14), 1: (1, 15, 2), 3: (1, 15, 14), 2: (1, 15)}[j]
        for d in to:
            second_a[j, d] = send(wall.at[y, rr, kk], wall.at[y, rr, kk], zd(d))
        to_y(rr, kk)
        return to

    def landed(j, to):
        for d in to:
            second_a[j, d].wait_recv()
            to_y(*block(d, j))

    landed(0, around(0))
    to = {}
    for j in (1, 3):
        first_b[j].wait_recv()
        to[j] = around(j)
    pass_on(1)
    landed(1, to[1])
    landed(3, to[3])
    pass_on(4)
    first_b[2].wait_recv()
    to = around(2)
    pass_on(2)
    landed(2, to)
    pass_on(9)
    for x in onward:
        x.wait_recv()
    for k in range(4):
        for rr in range(4):
            at = 96 * (4 * k + rr)
            out = []
            for yy in range(4):
                v = wall[yy, rr, k].astype(F32)
                out.append(jnp.concatenate([unpack(v[:, 0:384]), unpack(v[:, 384:768])], axis=1))
            wc_o[at:at + 96, :] = jnp.concatenate(out, axis=0).astype(BF16)
    assert len(copies) <= N_SEM
    for x in copies:
        x.wait_send()


def finish(small, wc, nw_o, up_o, nf_o, ns_o, wc_o):
    up_o[...] = small[0:24, :]
    nw_o[...] = small[24:48, :]
    nf_o[...] = small[48:52, :]
    ns_o[...] = small[52:56, :]
    wc_o[...] = wc[...]


def per_device(*args):
    v = pl.BlockSpec(memory_space=pltpu.VMEM)
    shape = jax.ShapeDtypeStruct
    small, wc = pl.pallas_call(
        kernel,
        name="step",
        out_shape=(shape((56, 512), F32), shape((1536, 512), BF16)),
        in_specs=[pl.BlockSpec(memory_space=pl.ANY)] * 6,
        out_specs=[v] * 2,
        scratch_shapes=[
            pltpu.VMEM((1024, 1536), BF16),
            pltpu.VMEM((1024, 512), BF16),
            pltpu.VMEM((24, 256), BF16),
            pltpu.VMEM((24, 512), F32),
            pltpu.VMEM((2, 4, 4, 512), F32),
            pltpu.VMEM((4, 384, 1024), BF16),
            pltpu.VMEM((2, 1536, 256), F32),
            pltpu.VMEM((2, 1536, 256), BF16),
            pltpu.VMEM((2, 2, 192, 256), BF16),
            pltpu.VMEM((2, 2, 192, 256), BF16),
            pltpu.VMEM((2, 2, 192, 256), BF16),
            pltpu.VMEM((2, 2, 192, 256), BF16),
            pltpu.VMEM((2, 384, 256), F32),
            pltpu.VMEM((2, 384, 256), BF16),
            pltpu.VMEM((2, 3, 96, 256), BF16),
            pltpu.VMEM((2, 96, 256), F32),
            pltpu.VMEM((2, 4, 16, 384), BF16),
            pltpu.VMEM((2, 3, 16, 384), BF16),
            pltpu.VMEM((4, 4, 16, 384), BF16),
            pltpu.VMEM((384, 256), F32),
            pltpu.VMEM((2, 256, 256), F32),
            pltpu.VMEM((2, 256, 256), BF16),
            pltpu.VMEM((2, 3, 64, 256), BF16),
            pltpu.VMEM((2, 64, 256), F32),
            pltpu.VMEM((2, 3, 16, 256), F32),
            pltpu.VMEM((2, 4, 16, 256), F32),
            pltpu.VMEM((4, 4, 512), F32),
            pltpu.VMEM((4, 4, 512), F32),
            pltpu.VMEM((2, 4, 4, 16, 512), BF16),
            pltpu.VMEM((2, 16, 512), F32),
            pltpu.VMEM((8, 2, 8, 128), F32),
            pltpu.VMEM((4, 2, 8, 128), F32),
            pltpu.VMEM((4, 2, 8, 128), F32),
            pltpu.VMEM((4, 4, 4, 16, 768), BF16),
            pltpu.SemaphoreType.DMA((9,)),
            pltpu.SemaphoreType.DMA((N_SEM,)),
            pltpu.SemaphoreType.DMA((N_SEM,)),
        ],
        compiler_params=pltpu.CompilerParams(collective_id=0, has_side_effects=True, vmem_limit_bytes=56 * 1024 * 1024),
    )(*args)
    return pl.pallas_call(
        finish,
        name="finish",
        out_shape=(shape((24, 512), F32), shape((24, 512), F32), shape((4, 512), F32), shape((4, 512), F32),
                   shape((1536, 512), BF16)),
        in_specs=[v] * 2,
        out_specs=[v] * 5,
    )(small, wc)


def solution(mesh):
    both = ("fs", "rep")
    in_specs = (P(both, None), P(both, "tp"), P(both, None), P(both, "tp"), P(both, "tp"), P(both, "tp"))
    out_specs = (P(both, "tp"), P(both, "tp"), P(both, "tp"), P(both, "tp"), P(None, "tp"))
    return jax.shard_map(per_device, mesh=mesh, in_specs=in_specs, out_specs=out_specs, check_vma=False)
```

```python
import jax
import jax.numpy as jnp
from jax import lax
from jax.experimental import pallas as pl
from jax.experimental.pallas import tpu as pltpu
from jax.sharding import PartitionSpec as P

MESH = pl.DeviceIdType.MESH
F32, BF16 = jnp.float32, jnp.bfloat16
WINDOW = ((1, 15, 2), (1, 15, 14))
YS = (1, 3, 2)
N_SEM = 224


def rows_dot(a, b):
    return lax.dot_general(a, b, (((0,), (0,)), ((), ())), preferred_element_type=F32)


def kernel(mixer_h, og_h, fac_h, w_h, m1_h, m2_h, out_o, wc_o,
           mixer, og, facy, fr, wv, wy, mv, my, mk, gf, sy, relay, direct, joined, landed_j, gy, sa, ra, ga, sb, rb,
           pp, rpa, pb, dall, pz, po, us, uo, sums, klass, wall, isem, ssem, rsem):
    z, y, t = lax.axis_index("fs"), lax.axis_index("rep"), lax.axis_index("tp")
    q, r = z // 4, lax.rem(z, 4)

    def zd(d):
        return {"fs": lax.rem(z + d, 16)}

    def yd(d):
        return {"rep": lax.rem(y + d, 4)}

    def td(d):
        return {"tp": lax.rem(t + d, 8)}

    def zyd(dz, dy):
        return {"fs": lax.rem(z + dz, 16), "rep": lax.rem(y + dy, 4)}

    copies = []

    def send(src, dst, dev):
        i = len(copies)
        c = pltpu.make_async_remote_copy(src_ref=src, dst_ref=dst, send_sem=ssem.at[i], recv_sem=rsem.at[i],
                                         device_id=dev, device_id_type=MESH)
        c.start()
        copies.append(c)
        return c

    def lanes(yy):
        return pl.ds(pl.multiple_of(yy * 128, 128), 128)

    barrier = pltpu.get_barrier_semaphore()
    peers = [zd(d) for d in (1, 15, 2, 14, 3, 13, 4, 12, 8)] + [yd(d) for d in YS] + [td(d) for d in range(1, 8)]
    peers += [zyd(dz, dy) for dz in (1, 15, 2, 14) for dy in YS]
    for dev in peers:
        pl.semaphore_signal(barrier, inc=1, device_id=dev, device_id_type=MESH)

    def load(i, src, dst):
        c = pltpu.make_async_copy(src, dst, isem.at[i])
        c.start()
        return c

    tiles = [pl.ds(384 * k, 384) for k in range(4)]
    in_og = load(0, og_h, og)
    in_mixer = [load(1 + k, mixer_h.at[:, tiles[k]], mixer.at[:, tiles[k]]) for k in range(4)]
    in_small = [load(5, fac_h, facy.at[y]), load(6, m1_h, mv.at[0]), load(7, m2_h, mv.at[1]), load(8, w_h, wv),
                load(9, m1_h.at[:, lanes(y)], my.at[0, y]), load(10, m2_h.at[:, lanes(y)], my.at[1, y]),
                load(11, w_h.at[:, lanes(y)], wy.at[y])]

    def partial(k):
        in_mixer[k].wait()
        tile = rows_dot(mixer[:, tiles[k]], og[...])
        for rr in range(4):
            for yy in range(4):
                v = tile[96 * rr:96 * rr + 96, 128 * yy:128 * yy + 128]
                gf[yy, k, rr] = v
                sy[yy, k, rr] = v.astype(BF16)

    in_og.wait()
    partial(0)
    partial(1)
    for x in in_small:
        x.wait()
    pl.semaphore_wait(barrier, len(peers))

    def at_y(d):
        return lax.rem(y + d, 4)

    def step_one(c):
        up = [send(sy.at[at_y(2), 2 * c], relay.at[c, 0], yd(1)), send(sy.at[at_y(1), 2 * c + 1], direct.at[c, 0], yd(1))]
        down = [send(sy.at[at_y(2), 2 * c + 1], relay.at[c, 1], yd(3)), send(sy.at[at_y(3), 2 * c], direct.at[c, 1], yd(3))]
        return up[0], down[0], up[1], down[1]

    def step_two(c, first):
        out = []
        for i, d in ((0, 1), (1, 3)):
            first[i].wait_recv()
            joined[c, i] = (gf[at_y(d), 2 * c + i] + relay[c, i].astype(F32)).astype(BF16)
            out.append(send(joined.at[c, i], landed_j.at[c, i], yd(d)))
        return list(first[2:]) + out

    fy = [send(facy.at[y], facy.at[y], yd(d)) for d in YS]
    ones, twos = [step_one(0), None], [None, None]
    my_copies = [send(mv.at[p, :, lanes(at_y(d))], my.at[p, y], yd(d)) for p in range(2) for d in YS]
    partial(2)
    partial(3)
    ones[1] = step_one(1)
    for x in fy:
        x.wait_recv()
    fz = jnp.concatenate([facy[yy].astype(F32) for yy in range(4)], axis=0).astype(BF16)
    fr[q] = fz
    fb = [send(fr.at[q], fr.at[q], zd(4 * j)) for j in (2, 1, 3)]
    twos[0] = step_two(0, ones[0])
    for x in my_copies:
        x.wait_recv()
    for p in range(2):
        for yy in range(4):
            mk[p, q, 4 * yy:4 * yy + 4, :] = my[p, yy]
    mb = [send(mk.at[p, q], mk.at[p, q], zd(4 * j)) for j in (2, 1, 3) for p in range(2)]
    twos[1] = step_two(1, ones[1])
    wy_copies = [send(wv.at[:, lanes(at_y(d))], wy.at[y], yd(d)) for d in YS]

    ga_copies = []
    for c in range(2):
        for x in twos[c]:
            x.wait_recv()
        for k, i, other in ((2 * c, 0, 1), (2 * c + 1, 1, 0)):
            total = gf[y, k] + landed_j[c, i].astype(F32) + direct[c, other].astype(F32)
            gy[k] = total
            sa[k] = total.astype(BF16)
        ga_copies.append([send(sa.at[pl.ds(2 * c, 2), lax.rem(z + d, 4)], ra.at[c, j], zd(d))
                          for j, d in enumerate(WINDOW[c])])

    for x in fb:
        x.wait_recv()
    part = None
    for c in range(2):
        for x in ga_copies[c]:
            x.wait_recv()
        for i in range(2):
            k = 2 * c + i
            total = gy[k, r]
            for j in range(3):
                total = total + ra[c, j, i].astype(F32)
            ga[k] = total
            low = total.astype(BF16)
            sb[k] = low
            add = rows_dot(fr[k], low) + rows_dot(fr[k], (total - low.astype(F32)).astype(BF16))
            part = add if part is None else part + add
    pp[...] = part.reshape(4, 4, 16, 128)
    pa_copies = [[send(pp.at[pl.ds(2 * h, 2), lax.rem(z + d, 4)], rpa.at[h, j], zd(d)) for j, d in enumerate(WINDOW[h])]
                 for h in range(2)]
    for h in range(2):
        for x in pa_copies[h]:
            x.wait_recv()
        for i in range(2):
            k = 2 * h + i
            pb[q, k] = (pp[k, r] + rpa[h, 0, i] + rpa[h, 1, i] + rpa[h, 2, i]).astype(BF16)
    pb_copies = [send(pb.at[q], pb.at[q], zd(4 * j)) for j in (2, 1, 3)]
    gb_copies = [send(sb.at[lax.rem(q + j, 4)], rb.at[j - 1], zd(4 * j)) for j in (2, 1, 3)]
    for x in mb:
        x.wait_recv()
    for x in pb_copies:
        x.wait_recv()
    proj = [jnp.concatenate([pb[i, k].astype(F32) for k in range(4)], axis=0) for i in range(4)]
    proj = ((proj[0] + proj[1]) + proj[2]) + proj[3]
    first = 0.8 * mk[0].reshape(64, 128) + 0.2 * proj
    second = 0.9 * mk[1].reshape(64, 128) + 0.1 * proj * proj
    low = [(first / (jnp.sqrt(second) + 1e-08)).astype(BF16), proj.astype(BF16)]
    for p in range(2):
        for k in range(4):
            dall[p, k, r] = low[p][16 * k:16 * k + 16]
        wide = low[p].astype(F32)
        sums[t, p] = jnp.sum((wide * wide).reshape(8, 8, 128), axis=0)
    st = [send(sums.at[t], sums.at[t], td(d)) for d in range(1, 8)]
    da = [send(dall.at[p, :, r], dall.at[p, :, r], zd(d)) for d in (1, 15) for p in range(2)]
    for d, at in ((2, 0), (14, 2)):
        for p in range(2):
            here = dall.at[p, pl.ds(at, 2), r]
            da.append(send(here, here, zd(d)))
    for k in range(4):
        for yy in range(4):
            pz[k, yy] = proj[16 * k + 4 * yy:16 * k + 4 * yy + 4]
    po[y] = pz[q, y]
    po_copies = [send(pz.at[q, at_y(d)], po.at[y], yd(d)) for d in YS]

    for x in st:
        x.wait_recv()
    s = sums[0]
    for i in range(1, 8):
        s = s + sums[i]
    klass[r, y] = s
    kl_copies = [send(klass.at[r, y], klass.at[r, y], zyd(dz, dy)) for dz in (2, 1, 15, 0) for dy in (2, 1, 3, 0)
                 if dz or dy]

    for x in wy_copies:
        x.wait_recv()
    weight = jnp.concatenate([wy[yy] for yy in range(4)], axis=0)
    for x in gb_copies:
        x.wait_recv()
    grad = ga[q]
    for j in range(3):
        grad = grad + rb[j].astype(F32)
    for x in da:
        x.wait_recv()
    back_dir = jnp.dot(fz, dall[0].reshape(256, 128), preferred_element_type=F32)
    back_proj = jnp.dot(fz, dall[1].reshape(256, 128), preferred_element_type=F32)
    for x in kl_copies:
        x.wait_recv()
    s = None
    for rr in range(4):
        for yy in range(4):
            s = klass[rr, yy] if s is None else s + klass[rr, yy]
    totals = [jnp.sum(jnp.sum(s[p], axis=1, keepdims=True), axis=0, keepdims=True) for p in range(2)]
    scale = jnp.sqrt(totals[0]) / jnp.sqrt(totals[1] + 1e-06)
    update = back_dir + scale * (grad - back_proj)
    wall[y, r, q] = (weight - 0.01 * update).astype(BF16)

    def of(delta):
        zz = lax.rem(z + 32 - delta, 16)
        return lax.rem(zz, 4), zz // 4

    spread, onward = [], []

    def to_y(rr, kk):
        here = wall.at[y, rr, kk]
        spread.append((send(here, here, yd(1)), send(here, here, yd(3)), rr, kk))

    def pass_on(n):
        for _ in range(n):
            i = len(onward)
            up, down, rr, kk = spread[i]
            for c in (up, down):
                c.wait_recv()
            here = wall.at[at_y(1 if i % 2 else 3), rr, kk]
            onward.append(send(here, here, yd(3 if i % 2 else 1)))

    near, far = {}, {}
    to_y(r, q)
    for m in (1, 4, 2, 3):
        for way in (1, -1):
            near[way, m] = send(wall.at[y, r, q], wall.at[y, r, q], zd(16 + way * m))
    for yy in range(4):
        us[yy] = update[24 * yy:24 * yy + 24]
    uo[y] = us[y]

    def landed(m):
        for way in (1, -1):
            near[way, m].wait_recv()
            rr, kk = of(4 * way)
            for n in (4, 1, 2, 3) if m == 4 else ():
                here = wall.at[y, rr, kk] if n < 4 else wall.at[y, rr, kk, pl.ds(24 - 24 * way, 48)]
                far[way, n] = send(here, here, zd(16 + way * n))
            to_y(*of(m * way))

    landed(1)
    landed(2)
    uo_copies = [send(us.at[at_y(d)], uo.at[y], yd(d)) for d in YS]
    landed(4)
    landed(3)
    pass_on(1)
    for n in (1, 2, 3):
        for way in (1, -1):
            far[way, n].wait_recv()
            to_y(*of((n + 4) * way))
        pass_on(2)
    for way in (1, -1):
        far[way, 4].wait_recv()
    to_y(*of(8))

    for x in uo_copies + po_copies:
        x.wait_recv()
    mine = jnp.concatenate([uo[yy] for yy in range(4)], axis=1)
    out_o[0:24, :] = mine
    out_o[24:48, :] = wv[...] - 0.01 * mine
    mine = jnp.concatenate([po[yy] for yy in range(4)], axis=1)
    out_o[48:52, :] = 0.8 * mv[0] + 0.2 * mine
    out_o[52:56, :] = 0.9 * mv[1] + 0.1 * mine * mine
    pass_on(9)
    for x in onward:
        x.wait_recv()
    for yy in range(4):
        for rr in range(4):
            for k in range(4):
                at = 96 * (4 * k + rr)
                wc_o[at:at + 96, 128 * yy:128 * yy + 128] = wall[yy, rr, k]
    assert len(copies) <= N_SEM
    for x in copies:
        x.wait_send()


def finish(small, wc, nw_o, up_o, nf_o, ns_o, wc_o):
    up_o[...] = small[0:24, :]
    nw_o[...] = small[24:48, :]
    nf_o[...] = small[48:52, :]
    ns_o[...] = small[52:56, :]
    wc_o[...] = wc[...]


def per_device(*args):
    v = pl.BlockSpec(memory_space=pltpu.VMEM)
    shape = jax.ShapeDtypeStruct
    small, wc = pl.pallas_call(
        kernel,
        name="step",
        out_shape=(shape((56, 512), F32), shape((1536, 512), BF16)),
        in_specs=[pl.BlockSpec(memory_space=pl.ANY)] * 6,
        out_specs=[v] * 2,
        scratch_shapes=[
            pltpu.VMEM((1024, 1536), BF16),
            pltpu.VMEM((1024, 512), BF16),
            pltpu.VMEM((4, 24, 256), BF16),
            pltpu.VMEM((4, 96, 256), BF16),
            pltpu.VMEM((24, 512), F32),
            pltpu.VMEM((4, 24, 128), F32),
            pltpu.VMEM((2, 4, 512), F32),
            pltpu.VMEM((2, 4, 4, 128), F32),
            pltpu.VMEM((2, 4, 16, 128), F32),
            pltpu.VMEM((4, 4, 4, 96, 128), F32),
            pltpu.VMEM((4, 4, 4, 96, 128), BF16),
            pltpu.VMEM((2, 2, 4, 96, 128), BF16),
            pltpu.VMEM((2, 2, 4, 96, 128), BF16),
            pltpu.VMEM((2, 2, 4, 96, 128), BF16),
            pltpu.VMEM((2, 2, 4, 96, 128), BF16),
            pltpu.VMEM((4, 4, 96, 128), F32),
            pltpu.VMEM((4, 4, 96, 128), BF16),
            pltpu.VMEM((2, 3, 2, 96, 128), BF16),
            pltpu.VMEM((4, 96, 128), F32),
            pltpu.VMEM((4, 96, 128), BF16),
            pltpu.VMEM((3, 96, 128), BF16),
            pltpu.VMEM((4, 4, 16, 128), F32),
            pltpu.VMEM((2, 3, 2, 16, 128), F32),
            pltpu.VMEM((4, 4, 16, 128), BF16),
            pltpu.VMEM((2, 4, 4, 16, 128), BF16),
            pltpu.VMEM((4, 4, 4, 128), F32),
            pltpu.VMEM((4, 4, 128), F32),
            pltpu.VMEM((4, 24, 128), F32),
            pltpu.VMEM((4, 24, 128), F32),
            pltpu.VMEM((8, 2, 8, 128), F32),
            pltpu.VMEM((4, 4, 2, 8, 128), F32),
            pltpu.VMEM((4, 4, 4, 96, 128), BF16),
            pltpu.SemaphoreType.DMA((12,)),
            pltpu.SemaphoreType.DMA((N_SEM,)),
            pltpu.SemaphoreType.DMA((N_SEM,)),
        ],
        compiler_params=pltpu.CompilerParams(collective_id=0, has_side_effects=True, vmem_limit_bytes=56 * 1024 * 1024),
    )(*args)
    return pl.pallas_call(
        finish,
        name="finish",
        out_shape=(shape((24, 512), F32), shape((24, 512), F32), shape((4, 512), F32), shape((4, 512), F32),
                   shape((1536, 512), BF16)),
        in_specs=[v] * 2,
        out_specs=[v] * 5,
    )(small, wc)


def solution(mesh):
    both = ("fs", "rep")
    in_specs = (P(both, None), P(both, "tp"), P(both, None), P(both, "tp"), P(both, "tp"), P(both, "tp"))
    out_specs = (P(both, "tp"), P(both, "tp"), P(both, "tp"), P(both, "tp"), P(None, "tp"))
    return jax.shard_map(per_device, mesh=mesh, in_specs=in_specs, out_specs=out_specs, check_vma=False)
```

```python
import jax
import jax.numpy as jnp
from jax import lax
from jax.experimental import pallas as pl
from jax.experimental.pallas import tpu as pltpu
from jax.sharding import PartitionSpec as P

MESH = pl.DeviceIdType.MESH
F32, BF16 = jnp.float32, jnp.bfloat16
WINDOW = ((1, 15, 2), (1, 15, 14))
YS = (1, 3, 2)
N_SEM = 224


def rows_dot(a, b):
    return lax.dot_general(a, b, (((0,), (0,)), ((), ())), preferred_element_type=F32)


def kernel(mixer_h, og_h, fac_h, w_h, m1_h, m2_h, out_o, wc_o,
           mixer, og, facy, fr, wv, wy, mv, my, mk, gf, sy, relay, direct, joined, landed_j, gy, sa, ra, ga, sb, rb,
           pp, rpa, pb, dall, pz, po, us, uo, sums, klass, wall, isem, far_in, ssem, rsem):
    z, y, t = lax.axis_index("fs"), lax.axis_index("rep"), lax.axis_index("tp")
    q, r = z // 4, lax.rem(z, 4)

    def zd(d):
        return {"fs": lax.rem(z + d, 16)}

    def yd(d):
        return {"rep": lax.rem(y + d, 4)}

    def td(d):
        return {"tp": lax.rem(t + d, 8)}

    def zyd(dz, dy):
        return {"fs": lax.rem(z + dz, 16), "rep": lax.rem(y + dy, 4)}

    copies = []

    def send(src, dst, dev):
        i = len(copies)
        c = pltpu.make_async_remote_copy(src_ref=src, dst_ref=dst, send_sem=ssem.at[i], recv_sem=rsem.at[i],
                                         device_id=dev, device_id_type=MESH)
        c.start()
        copies.append(c)
        return c

    def lanes(yy):
        return pl.ds(pl.multiple_of(yy * 128, 128), 128)

    barrier = pltpu.get_barrier_semaphore()
    peers = [zd(d) for d in (1, 15, 2, 14, 3, 13, 4, 12)] + [yd(d) for d in YS] + [td(d) for d in range(1, 8)]
    peers += [zyd(dz, dy) for dz in (1, 15, 2, 14) for dy in YS]
    for dev in peers:
        pl.semaphore_signal(barrier, inc=1, device_id=dev, device_id_type=MESH)

    def load(i, src, dst):
        c = pltpu.make_async_copy(src, dst, isem.at[i])
        c.start()
        return c

    tiles = [pl.ds(384 * k, 384) for k in range(4)]
    in_og = load(0, og_h, og)
    in_mixer = [load(1 + k, mixer_h.at[:, tiles[k]], mixer.at[:, tiles[k]]) for k in range(4)]
    in_small = [load(5, fac_h, facy.at[y]), load(6, m1_h, mv.at[0]), load(7, m2_h, mv.at[1]), load(8, w_h, wv),
                load(9, m1_h.at[:, lanes(y)], my.at[0, y]), load(10, m2_h.at[:, lanes(y)], my.at[1, y]),
                load(11, w_h.at[:, lanes(y)], wy.at[y])]

    def partial(k):
        in_mixer[k].wait()
        tile = rows_dot(mixer[:, tiles[k]], og[...])
        for rr in range(4):
            for yy in range(4):
                v = tile[96 * rr:96 * rr + 96, 128 * yy:128 * yy + 128]
                gf[yy, k, rr] = v
                sy[yy, k, rr] = v.astype(BF16)

    in_og.wait()
    partial(0)
    partial(1)
    for x in in_small:
        x.wait()
    pl.semaphore_wait(barrier, len(peers))
    pl.semaphore_signal(far_in, inc=1, device_id=zd(4), device_id_type=MESH)

    def at_y(d):
        return lax.rem(y + d, 4)

    halves = (pl.ds(0, 2), pl.ds(2, 2))

    def step_one(k):
        up = [send(sy.at[at_y(2), k, halves[0]], relay.at[k, 0], yd(1)), send(sy.at[at_y(1), k, halves[1]], direct.at[k, 0], yd(1))]
        down = [send(sy.at[at_y(2), k, halves[1]], relay.at[k, 1], yd(3)), send(sy.at[at_y(3), k, halves[0]], direct.at[k, 1], yd(3))]
        return up[0], down[0], up[1], down[1]

    def step_two(k, first):
        out = []
        for i, d in ((0, 1), (1, 3)):
            first[i].wait_recv()
            joined[k, i] = (gf[at_y(d), k, halves[i]] + relay[k, i].astype(F32)).astype(BF16)
            out.append(send(joined.at[k, i], landed_j.at[k, i], yd(d)))
        return list(first[2:]) + out

    fy = [send(facy.at[y], facy.at[y], yd(d)) for d in YS]
    ones, twos, ga_copies = [step_one(0), step_one(1)], [], []
    my_copies = [send(mv.at[p, :, lanes(at_y(d))], my.at[p, y], yd(d)) for p in range(2) for d in YS]
    partial(2)
    partial(3)
    for x in fy:
        x.wait_recv()
    fz = jnp.concatenate([facy[yy].astype(F32) for yy in range(4)], axis=0).astype(BF16)
    fr[q] = fz
    pl.semaphore_wait(far_in, 1)
    fb = [send(fr.at[q], fr.at[q], zd(4 * j)) for j in (2, 1, 3)]
    twos.append(step_two(0, ones[0]))
    ones.append(step_one(2))
    for x in my_copies:
        x.wait_recv()
    for p in range(2):
        for yy in range(4):
            mk[p, q, 4 * yy:4 * yy + 4, :] = my[p, yy]
    mb = [send(mk.at[p, q], mk.at[p, q], zd(4 * j)) for j in (2, 1, 3) for p in range(2)]
    twos.append(step_two(1, ones[1]))
    ones.append(step_one(3))

    def stage_a(k):
        for x in twos[k]:
            x.wait_recv()
        for i in range(2):
            total = gf[y, k, halves[i]] + landed_j[k, i].astype(F32) + direct[k, 1 - i].astype(F32)
            gy[k, halves[i]] = total
            sa[k, halves[i]] = total.astype(BF16)
        ga_copies.append([send(sa.at[k, lax.rem(z + d, 4)], ra.at[k, j], zd(d)) for j, d in enumerate(WINDOW[k % 2])])

    stage_a(0)
    twos.append(step_two(2, ones[2]))
    stage_a(1)
    twos.append(step_two(3, ones[3]))
    wy_copies = [send(wv.at[:, lanes(at_y(d))], wy.at[y], yd(d)) for d in YS]
    stage_a(2)
    stage_a(3)

    for x in fb:
        x.wait_recv()
    part = None
    for k in range(4):
        for x in ga_copies[k]:
            x.wait_recv()
        total = gy[k, r]
        for j in range(3):
            total = total + ra[k, j].astype(F32)
        ga[k] = total
        low = total.astype(BF16)
        sb[k] = low
        add = rows_dot(fr[k], low) + rows_dot(fr[k], (total - low.astype(F32)).astype(BF16))
        part = add if part is None else part + add
    pp[...] = part.reshape(4, 4, 16, 128)
    pa_copies = [[send(pp.at[pl.ds(2 * h, 2), lax.rem(z + d, 4)], rpa.at[h, j], zd(d)) for j, d in enumerate(WINDOW[h])]
                 for h in range(2)]
    for h in range(2):
        for x in pa_copies[h]:
            x.wait_recv()
        for i in range(2):
            k = 2 * h + i
            pb[q, k] = (pp[k, r] + rpa[h, 0, i] + rpa[h, 1, i] + rpa[h, 2, i]).astype(BF16)
    pb_copies = [send(pb.at[q], pb.at[q], zd(4 * j)) for j in (2, 1, 3)]
    gb_copies = [send(sb.at[lax.rem(q + j, 4)], rb.at[j - 1], zd(4 * j)) for j in (2, 1, 3)]
    for x in mb:
        x.wait_recv()
    for x in pb_copies:
        x.wait_recv()
    proj = [jnp.concatenate([pb[i, k].astype(F32) for k in range(4)], axis=0) for i in range(4)]
    proj = ((proj[0] + proj[1]) + proj[2]) + proj[3]
    first = 0.8 * mk[0].reshape(64, 128) + 0.2 * proj
    second = 0.9 * mk[1].reshape(64, 128) + 0.1 * proj * proj
    low = [(first / (jnp.sqrt(second) + 1e-08)).astype(BF16), proj.astype(BF16)]
    squares = []
    for p in range(2):
        for k in range(4):
            dall[p, k, r] = low[p][16 * k:16 * k + 16]
        wide = low[p].astype(F32)
        sq = jnp.sum((wide * wide).reshape(8, 8, 128), axis=0)
        squares.append(sq[0:4] + sq[4:8])
    sums[t] = jnp.concatenate(squares, axis=0)
    st = [send(sums.at[t], sums.at[t], td(d)) for d in range(1, 8)]
    da = [send(dall.at[p, :, r], dall.at[p, :, r], zd(d)) for d in (1, 15) for p in range(2)]
    for d, at in ((2, 0), (14, 2)):
        for p in range(2):
            here = dall.at[p, pl.ds(at, 2), r]
            da.append(send(here, here, zd(d)))
    for k in range(4):
        for yy in range(4):
            pz[k, yy] = proj[16 * k + 4 * yy:16 * k + 4 * yy + 4]
    po[y] = pz[q, y]
    po_copies = [send(pz.at[q, at_y(d)], po.at[y], yd(d)) for d in YS]

    for x in st:
        x.wait_recv()
    s = sums[0]
    for i in range(1, 8):
        s = s + sums[i]
    klass[r, y] = s
    kl_copies = [send(klass.at[r, y], klass.at[r, y], zyd(dz, dy)) for dz in (2, 1, 15, 0) for dy in (2, 1, 3, 0)
                 if dz or dy]

    for x in wy_copies:
        x.wait_recv()
    weight = jnp.concatenate([wy[yy] for yy in range(4)], axis=0)
    for x in gb_copies:
        x.wait_recv()
    grad = ga[q]
    for j in range(3):
        grad = grad + rb[j].astype(F32)
    for x in da:
        x.wait_recv()
    back_dir = jnp.dot(fz, dall[0].reshape(256, 128), preferred_element_type=F32)
    back_proj = jnp.dot(fz, dall[1].reshape(256, 128), preferred_element_type=F32)
    for x in kl_copies:
        x.wait_recv()
    s = None
    for rr in range(4):
        for yy in range(4):
            s = klass[rr, yy] if s is None else s + klass[rr, yy]
    totals = [jnp.sum(jnp.sum(s[4 * p:4 * p + 4], axis=1, keepdims=True), axis=0, keepdims=True) for p in range(2)]
    scale = jnp.sqrt(totals[0]) / jnp.sqrt(totals[1] + 1e-06)
    update = back_dir + scale * (grad - back_proj)
    wall[y, r, q] = (weight - 0.01 * update).astype(BF16)

    def of(delta):
        zz = lax.rem(z + 32 - delta, 16)
        return lax.rem(zz, 4), zz // 4

    spread, onward = [], []

    def to_y(rr, kk):
        here = wall.at[y, rr, kk]
        spread.append((send(here, here, yd(1)), send(here, here, yd(3)), rr, kk))

    def pass_on(n):
        for _ in range(n):
            i = len(onward)
            up, down, rr, kk = spread[i]
            for c in (up, down):
                c.wait_recv()
            here = wall.at[at_y(1 if i % 2 else 3), rr, kk]
            onward.append(send(here, here, yd(3 if i % 2 else 1)))

    near, far = {}, {}
    to_y(r, q)
    for m in (1, 4, 2, 3):
        for way in (1, -1):
            near[way, m] = send(wall.at[y, r, q], wall.at[y, r, q], zd(16 + way * m))
    for yy in range(4):
        us[yy] = update[24 * yy:24 * yy + 24]
    uo[y] = us[y]

    def landed(m):
        for way in (1, -1):
            near[way, m].wait_recv()
            rr, kk = of(4 * way)
            for n in (4, 1, 2, 3) if m == 4 else ():
                here = wall.at[y, rr, kk] if n < 4 else wall.at[y, rr, kk, pl.ds(24 - 24 * way, 48)]
                far[way, n] = send(here, here, zd(16 + way * n))
            to_y(*of(m * way))

    landed(1)
    landed(2)
    uo_copies = [send(us.at[at_y(d)], uo.at[y], yd(d)) for d in YS]
    landed(4)
    landed(3)
    pass_on(1)
    for n in (1, 2, 3):
        for way in (1, -1):
            far[way, n].wait_recv()
            to_y(*of((n + 4) * way))
        pass_on(2)
    for way in (1, -1):
        far[way, 4].wait_recv()
    to_y(*of(8))

    for x in uo_copies + po_copies:
        x.wait_recv()
    mine = jnp.concatenate([uo[yy] for yy in range(4)], axis=1)
    out_o[0:24, :] = mine
    out_o[24:48, :] = wv[...] - 0.01 * mine
    mine = jnp.concatenate([po[yy] for yy in range(4)], axis=1)
    out_o[48:52, :] = 0.8 * mv[0] + 0.2 * mine
    out_o[52:56, :] = 0.9 * mv[1] + 0.1 * mine * mine
    pass_on(9)
    for x in onward:
        x.wait_recv()
    for yy in range(4):
        for rr in range(4):
            for k in range(4):
                at = 96 * (4 * k + rr)
                wc_o[at:at + 96, 128 * yy:128 * yy + 128] = wall[yy, rr, k]
    assert len(copies) <= N_SEM
    for x in copies:
        x.wait_send()


def finish(small, wc, nw_o, up_o, nf_o, ns_o, wc_o, sem):
    moves = ((wc, wc_o), (small.at[0:24, :], up_o), (small.at[24:48, :], nw_o), (small.at[48:52, :], nf_o),
             (small.at[52:56, :], ns_o))
    copies = [pltpu.make_async_copy(src, dst, sem.at[i]) for i, (src, dst) in enumerate(moves)]
    for c in copies:
        c.start()
    for c in copies:
        c.wait()


def per_device(*args):
    v = pl.BlockSpec(memory_space=pltpu.VMEM)
    shape = jax.ShapeDtypeStruct
    small, wc = pl.pallas_call(
        kernel,
        name="step",
        out_shape=(pltpu.VMEM((56, 512), F32), pltpu.VMEM((1536, 512), BF16)),
        in_specs=[pl.BlockSpec(memory_space=pl.ANY)] * 6,
        out_specs=[v] * 2,
        scratch_shapes=[
            pltpu.VMEM((1024, 1536), BF16),
            pltpu.VMEM((1024, 512), BF16),
            pltpu.VMEM((4, 24, 256), BF16),
            pltpu.VMEM((4, 96, 256), BF16),
            pltpu.VMEM((24, 512), F32),
            pltpu.VMEM((4, 24, 128), F32),
            pltpu.VMEM((2, 4, 512), F32),
            pltpu.VMEM((2, 4, 4, 128), F32),
            pltpu.VMEM((2, 4, 16, 128), F32),
            pltpu.VMEM((4, 4, 4, 96, 128), F32),
            pltpu.VMEM((4, 4, 4, 96, 128), BF16),
            pltpu.VMEM((4, 2, 2, 96, 128), BF16),
            pltpu.VMEM((4, 2, 2, 96, 128), BF16),
            pltpu.VMEM((4, 2, 2, 96, 128), BF16),
            pltpu.VMEM((4, 2, 2, 96, 128), BF16),
            pltpu.VMEM((4, 4, 96, 128), F32),
            pltpu.VMEM((4, 4, 96, 128), BF16),
            pltpu.VMEM((4, 3, 96, 128), BF16),
            pltpu.VMEM((4, 96, 128), F32),
            pltpu.VMEM((4, 96, 128), BF16),
            pltpu.VMEM((3, 96, 128), BF16),
            pltpu.VMEM((4, 4, 16, 128), F32),
            pltpu.VMEM((2, 3, 2, 16, 128), F32),
            pltpu.VMEM((4, 4, 16, 128), BF16),
            pltpu.VMEM((2, 4, 4, 16, 128), BF16),
            pltpu.VMEM((4, 4, 4, 128), F32),
            pltpu.VMEM((4, 4, 128), F32),
            pltpu.VMEM((4, 24, 128), F32),
            pltpu.VMEM((4, 24, 128), F32),
            pltpu.VMEM((8, 8, 128), F32),
            pltpu.VMEM((4, 4, 8, 128), F32),
            pltpu.VMEM((4, 4, 4, 96, 128), BF16),
            pltpu.SemaphoreType.DMA((12,)),
            pltpu.SemaphoreType.REGULAR,
            pltpu.SemaphoreType.DMA((N_SEM,)),
            pltpu.SemaphoreType.DMA((N_SEM,)),
        ],
        compiler_params=pltpu.CompilerParams(collective_id=0, has_side_effects=True, vmem_limit_bytes=56 * 1024 * 1024),
    )(*args)
    return pl.pallas_call(
        finish,
        name="finish",
        out_shape=(shape((24, 512), F32), shape((24, 512), F32), shape((4, 512), F32), shape((4, 512), F32),
                   shape((1536, 512), BF16)),
        in_specs=[pl.BlockSpec(memory_space=pl.ANY)] * 2,
        out_specs=[pl.BlockSpec(memory_space=pl.ANY)] * 5,
        scratch_shapes=[pltpu.SemaphoreType.DMA((5,))],
    )(pltpu.with_memory_space_constraint(small, pltpu.VMEM), pltpu.with_memory_space_constraint(wc, pltpu.VMEM))


def solution(mesh):
    both = ("fs", "rep")
    in_specs = (P(both, None), P(both, "tp"), P(both, None), P(both, "tp"), P(both, "tp"), P(both, "tp"))
    out_specs = (P(both, "tp"), P(both, "tp"), P(both, "tp"), P(both, "tp"), P(None, "tp"))
    return jax.shard_map(per_device, mesh=mesh, in_specs=in_specs, out_specs=out_specs, check_vma=False)
```

```python
import jax
import jax.numpy as jnp
from jax import lax
from jax.experimental import pallas as pl
from jax.experimental.pallas import tpu as pltpu
from jax.sharding import PartitionSpec as P

MESH = pl.DeviceIdType.MESH
F32, BF16 = jnp.float32, jnp.bfloat16
WINDOW = ((1, 15, 2), (1, 15, 14))
YS = (1, 3, 2)
N_SEM = 224


def rows_dot(a, b):
    return lax.dot_general(a, b, (((0,), (0,)), ((), ())), preferred_element_type=F32)


def kernel(mixer_h, og_h, fac_h, w_h, m1_h, m2_h, out_o, wc_o,
           mixer, og, facy, fr, wv, wy, mv, my, mk, gf, sy, relay, direct, joined, landed_j, gy, sa, ra, ga, sb, rb,
           pp, rpa, pb, dall, pz, po, us, uo, sums, klass, wall, isem, far_in, ssem, rsem):
    z, y, t = lax.axis_index("fs"), lax.axis_index("rep"), lax.axis_index("tp")
    q, r = z // 4, lax.rem(z, 4)

    def zd(d):
        return {"fs": lax.rem(z + d, 16)}

    def yd(d):
        return {"rep": lax.rem(y + d, 4)}

    def td(d):
        return {"tp": lax.rem(t + d, 8)}

    def zyd(dz, dy):
        return {"fs": lax.rem(z + dz, 16), "rep": lax.rem(y + dy, 4)}

    copies = []

    def send(src, dst, dev):
        i = len(copies)
        c = pltpu.make_async_remote_copy(src_ref=src, dst_ref=dst, send_sem=ssem.at[i], recv_sem=rsem.at[i],
                                         device_id=dev, device_id_type=MESH)
        c.start()
        copies.append(c)
        return c

    def lanes(yy):
        return pl.ds(pl.multiple_of(yy * 128, 128), 128)

    barrier = pltpu.get_barrier_semaphore()
    peers = [zd(d) for d in (1, 15, 2, 14, 3, 13, 4, 12)] + [yd(d) for d in YS] + [td(d) for d in range(1, 8)]
    peers += [zyd(dz, dy) for dz in (1, 15, 2, 14) for dy in YS]
    for dev in peers:
        pl.semaphore_signal(barrier, inc=1, device_id=dev, device_id_type=MESH)

    def load(i, src, dst):
        c = pltpu.make_async_copy(src, dst, isem.at[i])
        c.start()
        return c

    tiles = [pl.ds(384 * k, 384) for k in range(4)]
    in_og = load(0, og_h, og)
    in_mixer = [load(1 + k, mixer_h.at[:, tiles[k]], mixer.at[:, tiles[k]]) for k in range(4)]
    in_small = [load(5, fac_h, facy.at[y]), load(6, m1_h, mv.at[0]), load(7, m2_h, mv.at[1]), load(8, w_h, wv),
                load(9, m1_h.at[:, lanes(y)], my.at[0, y]), load(10, m2_h.at[:, lanes(y)], my.at[1, y]),
                load(11, w_h.at[:, lanes(y)], wy.at[y])]

    def partial(k):
        in_mixer[k].wait()
        tile = rows_dot(mixer[:, tiles[k]], og[...])
        for rr in range(4):
            for yy in range(4):
                v = tile[96 * rr:96 * rr + 96, 128 * yy:128 * yy + 128]
                gf[yy, k, rr] = v
                sy[yy, k, rr] = v.astype(BF16)

    in_og.wait()
    partial(0)
    partial(1)
    for x in in_small:
        x.wait()
    pl.semaphore_wait(barrier, len(peers))
    pl.semaphore_signal(far_in, inc=1, device_id=zd(4), device_id_type=MESH)

    def at_y(d):
        return lax.rem(y + d, 4)

    halves = (pl.ds(0, 2), pl.ds(2, 2))

    def step_one(k):
        up = [send(sy.at[at_y(2), k, halves[0]], relay.at[k, 0], yd(1)), send(sy.at[at_y(1), k, halves[1]], direct.at[k, 0], yd(1))]
        down = [send(sy.at[at_y(2), k, halves[1]], relay.at[k, 1], yd(3)), send(sy.at[at_y(3), k, halves[0]], direct.at[k, 1], yd(3))]
        return up[0], down[0], up[1], down[1]

    def step_two(k, first):
        out = []
        for i, d in ((0, 1), (1, 3)):
            first[i].wait_recv()
            joined[k, i] = (gf[at_y(d), k, halves[i]] + relay[k, i].astype(F32)).astype(BF16)
            out.append(send(joined.at[k, i], landed_j.at[k, i], yd(d)))
        return list(first[2:]) + out

    fy = [send(facy.at[y], facy.at[y], yd(d)) for d in YS]
    ones, twos, ga_copies = [step_one(0), step_one(1)], [], []
    my_copies = [send(mv.at[p, :, lanes(at_y(d))], my.at[p, y], yd(d)) for p in range(2) for d in YS]
    partial(2)
    partial(3)
    for x in fy:
        x.wait_recv()
    fz = jnp.concatenate([facy[yy].astype(F32) for yy in range(4)], axis=0).astype(BF16)
    fr[q] = fz
    pl.semaphore_wait(far_in, 1)
    fb = [send(fr.at[q], fr.at[q], zd(4 * j)) for j in (2, 1, 3)]
    twos.append(step_two(0, ones[0]))
    ones.append(step_one(2))
    for x in my_copies:
        x.wait_recv()
    for p in range(2):
        for yy in range(4):
            mk[p, q, 4 * yy:4 * yy + 4, :] = my[p, yy]
    mb = [send(mk.at[p, q], mk.at[p, q], zd(4 * j)) for j in (2, 1, 3) for p in range(2)]
    twos.append(step_two(1, ones[1]))
    ones.append(step_one(3))

    def stage_a(k):
        for x in twos[k]:
            x.wait_recv()
        for i in range(2):
            total = gf[y, k, halves[i]] + landed_j[k, i].astype(F32) + direct[k, 1 - i].astype(F32)
            gy[k, halves[i]] = total
            sa[k, halves[i]] = total.astype(BF16)
        ga_copies.append([send(sa.at[k, lax.rem(z + d, 4)], ra.at[k, j], zd(d)) for j, d in enumerate(WINDOW[k % 2])])

    stage_a(0)
    twos.append(step_two(2, ones[2]))
    stage_a(1)
    twos.append(step_two(3, ones[3]))
    wy_copies = [send(wv.at[:, lanes(at_y(d))], wy.at[y], yd(d)) for d in YS]
    stage_a(2)
    stage_a(3)

    for x in fb:
        x.wait_recv()
    part = None
    for k in range(4):
        for x in ga_copies[k]:
            x.wait_recv()
        total = gy[k, r]
        for j in range(3):
            total = total + ra[k, j].astype(F32)
        ga[k] = total
        low = total.astype(BF16)
        sb[k] = low
        add = rows_dot(fr[k], low) + rows_dot(fr[k], (total - low.astype(F32)).astype(BF16))
        part = add if part is None else part + add
    pp[...] = part.reshape(4, 4, 16, 128)
    pa_copies = [[send(pp.at[pl.ds(2 * h, 2), lax.rem(z + d, 4)], rpa.at[h, j], zd(d)) for j, d in enumerate(WINDOW[h])]
                 for h in range(2)]
    for h in range(2):
        for x in pa_copies[h]:
            x.wait_recv()
        for i in range(2):
            k = 2 * h + i
            pb[q, k] = (pp[k, r] + rpa[h, 0, i] + rpa[h, 1, i] + rpa[h, 2, i]).astype(BF16)
    pb_copies = [send(pb.at[q], pb.at[q], zd(4 * j)) for j in (2, 1, 3)]
    gb_copies = [send(sb.at[lax.rem(q + j, 4)], rb.at[j - 1], zd(4 * j)) for j in (2, 1, 3)]
    for x in mb:
        x.wait_recv()
    for x in pb_copies:
        x.wait_recv()
    proj = [jnp.concatenate([pb[i, k].astype(F32) for k in range(4)], axis=0) for i in range(4)]
    proj = ((proj[0] + proj[1]) + proj[2]) + proj[3]
    first = 0.8 * mk[0].reshape(64, 128) + 0.2 * proj
    second = 0.9 * mk[1].reshape(64, 128) + 0.1 * proj * proj
    low = [(first / (jnp.sqrt(second) + 1e-08)).astype(BF16), proj.astype(BF16)]
    squares = []
    for p in range(2):
        for k in range(4):
            dall[p, k, r] = low[p][16 * k:16 * k + 16]
        wide = low[p].astype(F32)
        sq = jnp.sum((wide * wide).reshape(8, 8, 128), axis=0)
        squares.append(sq[0:4] + sq[4:8])
    sums[t] = jnp.concatenate(squares, axis=0)
    st = [send(sums.at[t], sums.at[t], td(d)) for d in range(1, 8)]
    da = [send(dall.at[p, :, r], dall.at[p, :, r], zd(d)) for d in (1, 15) for p in range(2)]
    for d, at in ((2, 0), (14, 2)):
        for p in range(2):
            here = dall.at[p, pl.ds(at, 2), r]
            da.append(send(here, here, zd(d)))
    for k in range(4):
        for yy in range(4):
            pz[k, yy] = proj[16 * k + 4 * yy:16 * k + 4 * yy + 4]
    po[y] = pz[q, y]
    po_copies = [send(pz.at[q, at_y(d)], po.at[y], yd(d)) for d in YS]

    for x in st:
        x.wait_recv()
    s = sums[0]
    for i in range(1, 8):
        s = s + sums[i]
    klass[r, y] = s
    kl_copies = [send(klass.at[r, y], klass.at[r, y], zyd(dz, dy)) for dz in (2, 1, 15, 0) for dy in (2, 1, 3, 0)
                 if dz or dy]

    for x in wy_copies:
        x.wait_recv()
    weight = jnp.concatenate([wy[yy] for yy in range(4)], axis=0)
    for x in gb_copies:
        x.wait_recv()
    grad = ga[q]
    for j in range(3):
        grad = grad + rb[j].astype(F32)
    for x in da:
        x.wait_recv()
    back_dir = jnp.dot(fz, dall[0].reshape(256, 128), preferred_element_type=F32)
    back_proj = jnp.dot(fz, dall[1].reshape(256, 128), preferred_element_type=F32)
    for x in kl_copies:
        x.wait_recv()
    s = None
    for rr in range(4):
        for yy in range(4):
            s = klass[rr, yy] if s is None else s + klass[rr, yy]
    totals = [jnp.sum(jnp.sum(s[4 * p:4 * p + 4], axis=1, keepdims=True), axis=0, keepdims=True) for p in range(2)]
    scale = jnp.sqrt(totals[0]) / jnp.sqrt(totals[1] + 1e-06)
    update = back_dir + scale * (grad - back_proj)
    wall[y, r, q] = (weight - 0.01 * update).astype(BF16)

    def of(delta):
        zz = lax.rem(z + 32 - delta, 16)
        return lax.rem(zz, 4), zz // 4

    spread, onward = [], []

    def to_y(rr, kk):
        here = wall.at[y, rr, kk]
        spread.append((send(here, here, yd(1)), send(here, here, yd(3)), rr, kk))

    def pass_on(n):
        for _ in range(n):
            i = len(onward)
            up, down, rr, kk = spread[i]
            for c in (up, down):
                c.wait_recv()
            here = wall.at[at_y(1 if i % 2 else 3), rr, kk]
            onward.append(send(here, here, yd(3 if i % 2 else 1)))

    near, far = {}, {}
    to_y(r, q)
    for m in (1, 4, 2, 3):
        for way in (1, -1):
            near[way, m] = send(wall.at[y, r, q], wall.at[y, r, q], zd(16 + way * m))
    for yy in range(4):
        us[yy] = update[24 * yy:24 * yy + 24]
    uo[y] = us[y]

    def landed(m):
        for way in (1, -1):
            near[way, m].wait_recv()
            rr, kk = of(4 * way)
            for n in (4, 1, 2, 3) if m == 4 else ():
                here = wall.at[y, rr, kk] if n < 4 else wall.at[y, rr, kk, pl.ds(24 - 24 * way, 48)]
                far[way, n] = send(here, here, zd(16 + way * n))
            to_y(*of(m * way))

    landed(1)
    landed(2)
    uo_copies = [send(us.at[at_y(d)], uo.at[y], yd(d)) for d in YS]
    landed(4)
    landed(3)
    pass_on(1)
    for n in (1, 2, 3):
        for way in (1, -1):
            far[way, n].wait_recv()
            to_y(*of((n + 4) * way))
        pass_on(2)
    for way in (1, -1):
        far[way, 4].wait_recv()
    to_y(*of(8))

    for x in uo_copies + po_copies:
        x.wait_recv()
    mine = jnp.concatenate([uo[yy] for yy in range(4)], axis=1)
    out_o[0:24, :] = mine
    out_o[24:48, :] = wv[...] - 0.01 * mine
    mine = jnp.concatenate([po[yy] for yy in range(4)], axis=1)
    out_o[48:52, :] = 0.8 * mv[0] + 0.2 * mine
    out_o[52:56, :] = 0.9 * mv[1] + 0.1 * mine * mine
    def write(d):
        for rr in range(4):
            for k in range(4):
                at = 96 * (4 * k + rr)
                wc_o[at:at + 96, lanes(at_y(d))] = wall[at_y(d), rr, k]

    write(0)
    pass_on(9)
    write(1)
    write(3)
    for x in onward:
        x.wait_recv()
    write(2)
    assert len(copies) <= N_SEM
    for x in copies:
        x.wait_send()


def finish(small, wc, nw_o, up_o, nf_o, ns_o, wc_o, sem):
    moves = ((wc, wc_o), (small.at[0:24, :], up_o), (small.at[24:48, :], nw_o), (small.at[48:52, :], nf_o),
             (small.at[52:56, :], ns_o))
    copies = [pltpu.make_async_copy(src, dst, sem.at[i]) for i, (src, dst) in enumerate(moves)]
    for c in copies:
        c.start()
    for c in copies:
        c.wait()


def per_device(*args):
    v = pl.BlockSpec(memory_space=pltpu.VMEM)
    shape = jax.ShapeDtypeStruct
    small, wc = pl.pallas_call(
        kernel,
        name="step",
        out_shape=(pltpu.VMEM((56, 512), F32), pltpu.VMEM((1536, 512), BF16)),
        in_specs=[pl.BlockSpec(memory_space=pl.ANY)] * 6,
        out_specs=[v] * 2,
        scratch_shapes=[
            pltpu.VMEM((1024, 1536), BF16),
            pltpu.VMEM((1024, 512), BF16),
            pltpu.VMEM((4, 24, 256), BF16),
            pltpu.VMEM((4, 96, 256), BF16),
            pltpu.VMEM((24, 512), F32),
            pltpu.VMEM((4, 24, 128), F32),
            pltpu.VMEM((2, 4, 512), F32),
            pltpu.VMEM((2, 4, 4, 128), F32),
            pltpu.VMEM((2, 4, 16, 128), F32),
            pltpu.VMEM((4, 4, 4, 96, 128), F32),
            pltpu.VMEM((4, 4, 4, 96, 128), BF16),
            pltpu.VMEM((4, 2, 2, 96, 128), BF16),
            pltpu.VMEM((4, 2, 2, 96, 128), BF16),
            pltpu.VMEM((4, 2, 2, 96, 128), BF16),
            pltpu.VMEM((4, 2, 2, 96, 128), BF16),
            pltpu.VMEM((4, 4, 96, 128), F32),
            pltpu.VMEM((4, 4, 96, 128), BF16),
            pltpu.VMEM((4, 3, 96, 128), BF16),
            pltpu.VMEM((4, 96, 128), F32),
            pltpu.VMEM((4, 96, 128), BF16),
            pltpu.VMEM((3, 96, 128), BF16),
            pltpu.VMEM((4, 4, 16, 128), F32),
            pltpu.VMEM((2, 3, 2, 16, 128), F32),
            pltpu.VMEM((4, 4, 16, 128), BF16),
            pltpu.VMEM((2, 4, 4, 16, 128), BF16),
            pltpu.VMEM((4, 4, 4, 128), F32),
            pltpu.VMEM((4, 4, 128), F32),
            pltpu.VMEM((4, 24, 128), F32),
            pltpu.VMEM((4, 24, 128), F32),
            pltpu.VMEM((8, 8, 128), F32),
            pltpu.VMEM((4, 4, 8, 128), F32),
            pltpu.VMEM((4, 4, 4, 96, 128), BF16),
            pltpu.SemaphoreType.DMA((12,)),
            pltpu.SemaphoreType.REGULAR,
            pltpu.SemaphoreType.DMA((N_SEM,)),
            pltpu.SemaphoreType.DMA((N_SEM,)),
        ],
        compiler_params=pltpu.CompilerParams(collective_id=0, has_side_effects=True, vmem_limit_bytes=56 * 1024 * 1024),
    )(*args)
    return pl.pallas_call(
        finish,
        name="finish",
        out_shape=(shape((24, 512), F32), shape((24, 512), F32), shape((4, 512), F32), shape((4, 512), F32),
                   shape((1536, 512), BF16)),
        in_specs=[pl.BlockSpec(memory_space=pl.ANY)] * 2,
        out_specs=[pl.BlockSpec(memory_space=pl.ANY)] * 5,
        scratch_shapes=[pltpu.SemaphoreType.DMA((5,))],
    )(pltpu.with_memory_space_constraint(small, pltpu.VMEM), pltpu.with_memory_space_constraint(wc, pltpu.VMEM))


def solution(mesh):
    both = ("fs", "rep")
    in_specs = (P(both, None), P(both, "tp"), P(both, None), P(both, "tp"), P(both, "tp"), P(both, "tp"))
    out_specs = (P(both, "tp"), P(both, "tp"), P(both, "tp"), P(both, "tp"), P(None, "tp"))
    return jax.shard_map(per_device, mesh=mesh, in_specs=in_specs, out_specs=out_specs, check_vma=False)
```
